32 devices in a mesh: ep: 8 (over z, y), tp: 4 (over x, core).
Axes of the slice: x: 2, y: 2, z: 4, core: 2. Of those that a mesh axis runs over, the one named last changes fastest.
Arguments:
- q_latent: bfloat16 [4096, 1024], P(('ep', 'tp')), may hold values from -6 to 6
- kv_latent: bfloat16 [4096, 512], P(('ep', 'tp')), may hold values from -8 to 8
- rope_key: bfloat16 [4096, 64], P(('ep', 'tp')), may hold values from -2500 to 2500
- gain_query: float32 [1024], replicated, may hold values from 0.1 to 1.9
- gain_latent: float32 [512], replicated, may hold values from 0.1 to 1.9
- w_query: bfloat16 [1024, 3072], P(None, 'tp'), may hold values from -0.1875 to 0.1875
- w_key: bfloat16 [512, 2048], P(None, 'tp'), may hold values from -0.625 to 0.625
- w_value: bfloat16 [512, 2048], P(None, 'tp'), may hold values from -0.25 to 0.25
- w_out: bfloat16 [2048, 4096], P('tp'), may hold values from -0.25 to 0.25
- tokens_b: bfloat16 [4096, 4096], P(('ep', 'tp')), may hold values from -6 to 6
- gain_norm: float32 [4096], replicated, may hold values from 0.1 to 1.9
- routes: int32 [4096, 2], P(('ep', 'tp')), may hold values from 0 to 7, all different within a row; in each aligned block of 128 rows (0 to 127, 128 to 255, ...) at most 40 rows name the same one
- route_weights: float32 [4096, 2], P(('ep', 'tp')), may hold values from 0.2 to 1
- shared_gate: bfloat16 [4096, 1024], P(None, 'tp'), may hold values from -0.09375 to 0.09375
- shared_up: bfloat16 [4096, 1024], P(None, 'tp'), may hold values from -0.09375 to 0.09375
- shared_down: bfloat16 [1024, 4096], P('tp'), may hold values from -0.1875 to 0.1875
- expert_gate: bfloat16 [8, 4096, 1024], P('ep', None, 'tp'), may hold values from -0.09375 to 0.09375
- expert_up: bfloat16 [8, 4096, 1024], P('ep', None, 'tp'), may hold values from -0.09375 to 0.09375
- expert_down: bfloat16 [8, 1024, 4096], P('ep', 'tp'), may hold values from -0.1875 to 0.1875
Outputs:
- mixer_out: bfloat16 [4096, 4096], P(('ep', 'tp'))
- expert_mix: bfloat16 [4096, 4096], P(('ep', 'tp'))
The draws below stay inside these ranges and needn't reach their ends.
Inputs may be any that keep to these rules, and one draw needn't show every extreme that they name: `routes`: in each aligned block of 128 rows no expert is named by more than 40 rows.
All inputs are finite; a program needn't handle non-finite values.
Results may differ from the reference program's by a relative error of at most 0.018.
The reference program's roundings to bfloat16 on the way count: a program that leaves them out, or rounds other values in their place, can miss the bound.
Values may be sent and summed in bfloat16 or wider, within the bound.
A program may use at most 192 MiB of HBM per device.

```python
import math
import jax
import jax.numpy as jnp
import numpy as np
from jax import lax

D = 4096
HEADS = 16
NOPE = 128
ROPE = 64
VDIM = 128
QLAT = 1024
KVLAT = 512
FF = 1024
TOP_K = 2
TOK_DEV = 128
EXPERTS = 8
CAPQ = 40
TOKENS = 4096
LENGTH = 4096
N_TP = 4


def draw_rope_key(key, part):
    normal_rows = jnp.clip(jax.random.normal(key, (TOKENS, ROPE), jnp.float32), -6.0, 6.0)
    return normal_rows.astype(jnp.bfloat16)


def draw_kv_latent(key, part):
    noise_key, common_key = jax.random.split(jax.random.fold_in(key, 5))
    block_total = TOKENS // TOK_DEV
    common = jnp.clip(jax.random.normal(common_key, (block_total, KVLAT), jnp.float32), -3.0, 3.0)
    noise = 0.8 * jnp.clip(jax.random.normal(noise_key, (TOKENS, KVLAT), jnp.float32), -6.0, 6.0)
    rows = noise + jnp.repeat(common, TOK_DEV, axis=0)
    return rows.astype(jnp.bfloat16)


def level_of(stream_key, shape, cuts, low, high):
    def one(axis_at, shards_of):
        steps = jax.random.uniform(jax.random.fold_in(jax.random.fold_in(stream_key, 6), axis_at), (shards_of,), jnp.float32, low / len(cuts), high / len(cuts))
        return jnp.repeat(jnp.exp(steps), shape[axis_at] // shards_of).reshape((-1,) + (1,) * (len(shape) - axis_at - 1))

    loudness = one(*cuts[0])
    for cut in cuts[1:]:
        loudness = loudness * one(*cut)
    return loudness


def shared_out(key, own, number, rows, number_of, top, most, skew):
    ranking = jax.random.permutation(key, number_of)
    packed, usual = shares(number_of, rows * top, most, skew, True), shares(number_of, rows * top, most, skew, False)
    places = jnp.arange(number_of)

    def named(tallies, offset_by):
        used = int((tallies > 0).sum())
        fixed = max(1, used // 4)
        shifted = fixed + (places - fixed + offset_by * (used - fixed)) % max(1, number_of - fixed)
        return jnp.zeros((number_of,), jnp.int32).at[ranking[jnp.where(places < fixed, places, shifted)]].set(jnp.asarray(tallies, jnp.int32))

    tallies = jnp.where(number % 4 == 0, named(packed, number // 4), named(usual, number - number // 4 - 1))
    mixed = jax.random.permutation(jax.random.fold_in(own, 3), number_of)
    source_of, taker = mixed[0:number_of // 2 * 2:2], mixed[1:number_of // 2 * 2:2]
    slack = jnp.minimum(tallies[source_of] - 1, most - tallies[taker]) // 2
    slack = jnp.where((source_of == ranking[0]) | (taker == ranking[0]) | (tallies[taker] == 0), 0, jnp.maximum(slack, 0))
    shifted = jax.random.randint(jax.random.fold_in(own, 4), (number_of // 2,), 0, 1 << 20) % (slack + 1)
    tallies = tallies.at[source_of].add(-shifted).at[taker].add(shifted)
    items = jnp.searchsorted(jnp.cumsum(tallies), jnp.arange(rows * top), side="right").astype(jnp.int32)
    listing = items.reshape(top, rows).T
    listing = listing[jax.random.permutation(jax.random.fold_in(own, 1), rows)]
    offset_by = jax.random.randint(jax.random.fold_in(own, 2), (rows, 1), 0, top)
    return jnp.take_along_axis(listing, (jnp.arange(top)[None, :] + offset_by) % top, axis=1)


def shares(count, total, most, slope, full):
    loads = [(1 << 20) // math.isqrt(standing ** slope) + 1 for standing in range(1, count + 1)]
    largest = most if full else min(most, max(-(-total // count), total * loads[0] // sum(loads)))
    least = 1 if total - largest >= count - 1 else 0
    given, spare = [largest] + [least] * (count - 1), total - largest - least * (count - 1)
    while spare > 0:
        candidates = [i for i in range(1, count) if given[i] < largest] or [i for i in range(1, count) if given[i] < most]
        whole, remaining = sum([loads[i] for i in candidates]), spare
        for i in candidates:
            more = min(most - given[i], max(1, remaining * loads[i] // whole), spare)
            given[i] = given[i] + more
            spare = spare - more
    return np.array(given)


def bell_draw(own_key, extent, spread, reach, cuts=(), kind=jnp.bfloat16):
    values = spread * jax.random.normal(own_key, extent, jnp.float32)
    if cuts:
        values = values * level_of(own_key, extent, cuts, -0.22, 0.18)
    return jnp.clip(values, -reach, reach).astype(kind)


def setup_inputs(seed: int = 0) -> dict:
    key_list = jax.random.split(jax.random.key(seed), 20)
    q_latent = bell_draw(key_list[0], (TOKENS, QLAT), 1.0, 6.0, ((0, 32),))
    kv_latent = draw_kv_latent(jax.random.fold_in(key_list[19], 71), 0)
    rope_key = draw_rope_key(jax.random.fold_in(key_list[19], 71), 0)
    gain_query = jnp.clip(1.0 + 0.18 * jax.random.normal(key_list[3], (QLAT,), jnp.float32), 0.1, 1.9)
    gain_latent = jnp.clip(1.0 + 0.18 * jax.random.normal(key_list[4], (KVLAT,), jnp.float32), 0.1, 1.9)
    w_query = bell_draw(key_list[5], (QLAT, HEADS * (NOPE + ROPE)), QLAT ** -0.5, 0.1875, ((1, 4),))
    w_key = bell_draw(key_list[6], (KVLAT, HEADS * NOPE), (KVLAT // 6) ** -0.5, 0.625, ((1, 4),))
    w_value = bell_draw(key_list[7], (KVLAT, HEADS * VDIM), KVLAT ** -0.5, 0.25, ((1, 4),))
    w_out = bell_draw(key_list[8], (HEADS * VDIM, D), (HEADS * VDIM // 4) ** -0.5, 0.25, ((0, 4),))
    tokens_b = bell_draw(key_list[9], (TOKENS, D), 1.0, 6.0, ((0, 32),))
    gain_norm = jnp.clip(1.0 + 0.18 * jax.random.normal(key_list[10], (D,), jnp.float32), 0.1, 1.9)
    routes_keys = jax.random.split(jax.random.fold_in(key_list[11], 1), TOKENS // TOK_DEV)
    routes_turns = jax.random.permutation(jax.random.fold_in(key_list[11], 3), TOKENS // TOK_DEV)
    routes = jax.vmap(lambda own, number: shared_out(jax.random.fold_in(key_list[11], 2), own, number, TOK_DEV, EXPERTS, TOP_K, CAPQ, 1))(routes_keys, routes_turns).reshape((TOKENS, TOP_K))
    route_weights = jnp.clip(jnp.exp(math.log(1.0) - 1.609438 * jax.random.uniform(key_list[12], (TOKENS, TOP_K), jnp.float32) ** level_of(key_list[12], (TOKENS, TOP_K), ((0, 32),), -0.2, 0.2)), 0.2, 1.0)
    shared_gate = bell_draw(key_list[13], (D, FF), D ** -0.5, 0.09375, ((1, 4),))
    shared_up = bell_draw(key_list[14], (D, FF), D ** -0.5, 0.09375, ((1, 4),))
    shared_down = bell_draw(key_list[15], (FF, D), FF ** -0.5, 0.1875, ((0, 4),))
    expert_gate = bell_draw(key_list[16], (EXPERTS, D, FF), D ** -0.5, 0.09375, ((0, 8), (2, 4)))
    expert_up = bell_draw(key_list[17], (EXPERTS, D, FF), D ** -0.5, 0.09375, ((0, 8), (2, 4)))
    expert_down = bell_draw(key_list[18], (EXPERTS, FF, D), FF ** -0.5, 0.1875, ((0, 8), (1, 4)))
    return dict(q_latent=q_latent, kv_latent=kv_latent, rope_key=rope_key, gain_query=gain_query, gain_latent=gain_latent, w_query=w_query, w_key=w_key, w_value=w_value, w_out=w_out, tokens_b=tokens_b, gain_norm=gain_norm, routes=routes, route_weights=route_weights, shared_gate=shared_gate, shared_up=shared_up, shared_down=shared_down, expert_gate=expert_gate, expert_up=expert_up, expert_down=expert_down)


epsilon = 1e-06
rope_theta = 10000.0

def rms_scale(values, gain_vec):
    floats = values.astype(jnp.float32)
    scaled = floats * lax.rsqrt(lax.optimization_barrier(jnp.mean(floats * floats, axis=-1, keepdims=True)) + epsilon)
    return (scaled * gain_vec).astype(jnp.bfloat16)

def rope_angles(positions, rope_width):
    frequency = rope_theta ** (-jnp.arange(0, rope_width, 2, dtype=jnp.float32) / rope_width)
    angles = positions.astype(jnp.float32)[:, None] * frequency[None, :]
    return (jnp.cos(angles), jnp.sin(angles))

def rotate_pairs(values, cos_tab, sin_tab):
    half_width = values.shape[-1] // 2
    first_half = values[..., :half_width]
    second_half = values[..., half_width:]
    return jnp.concatenate([first_half * cos_tab - second_half * sin_tab, second_half * cos_tab + first_half * sin_tab], axis=-1)

def rounded(values):
    return lax.optimization_barrier(values.astype(jnp.bfloat16)).astype(jnp.float32)

def group_sum(hidden, down_weight):
    row_total = hidden.shape[0]
    hidden_groups = hidden.reshape(row_total, N_TP, -1)
    down_groups = down_weight.reshape(N_TP, -1, down_weight.shape[-1])
    running_sum = jnp.zeros((row_total, down_weight.shape[-1]), jnp.float32)
    for group_num in range(N_TP):
        partial_value = jnp.dot(hidden_groups[:, group_num], down_groups[group_num], preferred_element_type=jnp.float32)
        running_sum = running_sum + rounded(partial_value)
    return running_sum.astype(jnp.bfloat16)

def reference(q_latent, kv_latent, rope_key, gain_query, gain_latent, w_query, w_key, w_value, w_out, tokens_b, gain_norm, routes, route_weights, shared_gate, shared_up, shared_down, expert_gate, expert_up, expert_down):
    q_normed = rms_scale(q_latent, gain_query)
    kv_normed = rms_scale(kv_latent, gain_latent)
    positions = jnp.arange(TOKENS, dtype=jnp.int32) % LENGTH
    cos_tab, sin_tab = rope_angles(positions, ROPE)
    query_full = jnp.dot(q_normed, w_query, preferred_element_type=jnp.float32).reshape(TOKENS, HEADS, NOPE + ROPE)
    query_rot = rotate_pairs(query_full[:, :, NOPE:], cos_tab[:, None, :], sin_tab[:, None, :])
    queries = jnp.concatenate([query_full[:, :, :NOPE], query_rot], axis=-1).astype(jnp.bfloat16)
    rot_keys = rotate_pairs(rope_key.astype(jnp.float32), cos_tab, sin_tab).astype(jnp.bfloat16)
    keys = jnp.dot(kv_normed, w_key, preferred_element_type=jnp.float32).astype(jnp.bfloat16).reshape(TOKENS, HEADS, NOPE)
    values = jnp.dot(kv_normed, w_value, preferred_element_type=jnp.float32).astype(jnp.bfloat16).reshape(TOKENS, HEADS, VDIM)
    block_rows = TOK_DEV * N_TP
    block_count = TOKENS // block_rows

    def attend_block(block_num):
        first_row = (block_num * block_rows).astype(jnp.int32)
        seq_first = (first_row // LENGTH * LENGTH).astype(jnp.int32)
        query_blk = lax.dynamic_slice_in_dim(queries, first_row, block_rows, 0).astype(jnp.float32)
        key_blk = lax.dynamic_slice_in_dim(keys, seq_first, LENGTH, 0).astype(jnp.float32)
        pe_blk = lax.dynamic_slice_in_dim(rot_keys, seq_first, LENGTH, 0).astype(jnp.float32)
        value_blk = lax.dynamic_slice_in_dim(values, seq_first, LENGTH, 0).astype(jnp.float32)
        scores = jnp.einsum('qhd,khd->hqk', query_blk[:, :, :NOPE], key_blk)
        scores = scores + jnp.einsum('qhr,kr->hqk', query_blk[:, :, NOPE:], pe_blk)
        scores = scores * (NOPE + ROPE) ** (-0.5)
        query_pos = first_row + jnp.arange(block_rows, dtype=jnp.int32)
        key_pos = seq_first + jnp.arange(LENGTH, dtype=jnp.int32)
        allowed = key_pos[None, :] <= query_pos[:, None]
        scores = jnp.where(allowed[None], scores, -jnp.inf)
        row_top = lax.optimization_barrier(jnp.max(scores, axis=-1, keepdims=True))
        exp_terms = jnp.exp(scores - row_top)
        denom_sum = lax.optimization_barrier(jnp.sum(exp_terms, axis=-1))
        weights = rounded(exp_terms)
        weighted = jnp.einsum('hqk,khd->qhd', weights, value_blk)
        return (weighted / denom_sum.T[:, :, None]).astype(jnp.bfloat16)
    heads_out = lax.map(attend_block, jnp.arange(block_count, dtype=jnp.int32)).reshape(TOKENS, HEADS * VDIM)
    mixer_out = group_sum(heads_out, w_out)
    normed_b = rms_scale(tokens_b, gain_norm)
    block_total = TOKENS // TOK_DEV
    pair_ids = routes.reshape(block_total, TOK_DEV * TOP_K).astype(jnp.int32)
    onehot = (pair_ids[:, :, None] == jnp.arange(EXPERTS, dtype=jnp.int32)[None, None, :]).astype(jnp.int32)
    slot_ids = lax.optimization_barrier(jnp.sum((jnp.cumsum(onehot, axis=1) - onehot) * onehot, axis=-1)).astype(jnp.int32)
    token_ids = jnp.repeat(jnp.arange(TOKENS, dtype=jnp.int32).reshape(block_total, TOK_DEV), TOP_K, axis=1)
    block_ids = jnp.broadcast_to(jnp.arange(block_total, dtype=jnp.int32)[:, None], pair_ids.shape)
    slot_table = jnp.full((EXPERTS, block_total, CAPQ), TOKENS, jnp.int32).at[pair_ids, block_ids, slot_ids].set(token_ids)
    padded = jnp.concatenate([normed_b, jnp.zeros((1, D), jnp.bfloat16)], axis=0)

    def run_expert(expert_num):
        chosen = jnp.take(padded, slot_table[expert_num].reshape(-1), axis=0)
        gate_act = jnp.dot(chosen, expert_gate[expert_num], preferred_element_type=jnp.float32)
        up_act = jnp.dot(chosen, expert_up[expert_num], preferred_element_type=jnp.float32)
        hidden = (jax.nn.silu(gate_act) * up_act).astype(jnp.bfloat16)
        return group_sum(hidden, expert_down[expert_num])
    expert_rows = lax.map(run_expert, jnp.arange(EXPERTS, dtype=jnp.int32))
    flat_index = (pair_ids * (block_total * CAPQ) + block_ids * CAPQ + slot_ids).reshape(-1).astype(jnp.int32)
    picked = jnp.take(expert_rows.reshape(-1, D), flat_index, axis=0).reshape(TOKENS, TOP_K, D)
    gate_shared = jnp.dot(normed_b, shared_gate, preferred_element_type=jnp.float32)
    up_shared = jnp.dot(normed_b, shared_up, preferred_element_type=jnp.float32)
    shared_hidden = (jax.nn.silu(gate_shared) * up_shared).astype(jnp.bfloat16)
    shared_result = group_sum(shared_hidden, shared_down)
    routed_sum = lax.optimization_barrier(jnp.sum(route_weights[:, :, None] * picked.astype(jnp.float32), axis=1))
    expert_mix = (shared_result.astype(jnp.float32) + routed_sum).astype(jnp.bfloat16)
    return (mixer_out, expert_mix)
```

```python
import functools

import jax
import jax.numpy as jnp
from jax import lax
from jax.experimental import pallas as pl
from jax.experimental.pallas import tpu as pltpu
from jax.sharding import PartitionSpec as P

NOPE = 128
ROPE = 64
VDIM = 128
SEQS = 1


epsilon = 1e-06
rope_theta = 10000.0


def exchange_kernel(axis, count, src_ref, dst_ref, send_sem, recv_sem, local_sem):
    me = lax.axis_index(axis)
    barrier = pltpu.get_barrier_semaphore()
    for step in range(1, count):
        pl.semaphore_signal(
            barrier,
            inc=1,
            device_id={axis: lax.rem(me + step, count)},
            device_id_type=pl.DeviceIdType.MESH,
        )
    pl.semaphore_wait(barrier, count - 1)
    copies = []
    for step in range(1, count):
        target = lax.rem(me + step, count)
        copy = pltpu.make_async_remote_copy(
            src_ref=src_ref.at[target],
            dst_ref=dst_ref.at[me],
            send_sem=send_sem.at[step],
            recv_sem=recv_sem.at[step],
            device_id={axis: target},
            device_id_type=pl.DeviceIdType.MESH,
        )
        copy.start()
        copies.append(copy)
    own = pltpu.make_async_copy(src_ref.at[me], dst_ref.at[me], local_sem)
    own.start()
    own.wait()
    for copy in copies:
        copy.wait()


def exchange(blocks, axis, collective_id):
    count = blocks.shape[0]
    return pl.pallas_call(
        functools.partial(exchange_kernel, axis, count),
        out_shape=jax.ShapeDtypeStruct(blocks.shape, blocks.dtype),
        in_specs=[pl.BlockSpec(memory_space=pltpu.VMEM)],
        out_specs=pl.BlockSpec(memory_space=pltpu.VMEM),
        scratch_shapes=[
            pltpu.SemaphoreType.DMA((count,)),
            pltpu.SemaphoreType.DMA((count,)),
            pltpu.SemaphoreType.DMA,
        ],
        compiler_params=pltpu.CompilerParams(
            collective_id=collective_id, has_side_effects=True, vmem_limit_bytes=16 * 2**20
        ),
        cost_estimate=pl.CostEstimate(
            flops=0, bytes_accessed=40 * blocks.size * 2, transcendentals=0
        ),
    )(blocks)


def rms_scale(values, gain_vec):
    floats = values.astype(jnp.float32)
    scaled = floats * lax.rsqrt(jnp.mean(floats * floats, axis=-1, keepdims=True) + epsilon)
    return (scaled * gain_vec).astype(jnp.bfloat16)


def rope_angles(positions, rope_width):
    frequency = rope_theta ** (-jnp.arange(0, rope_width, 2, dtype=jnp.float32) / rope_width)
    angles = positions.astype(jnp.float32)[:, None] * frequency[None, :]
    return (jnp.cos(angles), jnp.sin(angles))


def rotate_pairs(values, cos_tab, sin_tab):
    half_width = values.shape[-1] // 2
    first_half = values[..., :half_width]
    second_half = values[..., half_width:]
    return jnp.concatenate(
        [
            first_half * cos_tab - second_half * sin_tab,
            second_half * cos_tab + first_half * sin_tab,
        ],
        axis=-1,
    )


def block_scores(query_nope, query_rot, kv_block, pe_block, w_key, w_value, head_local):
    key_rows = kv_block.shape[0]
    key_proj = jnp.dot(kv_block, w_key, preferred_element_type=jnp.float32).astype(jnp.bfloat16)
    key_proj = key_proj.reshape(key_rows, head_local, -1)
    values = jnp.dot(kv_block, w_value, preferred_element_type=jnp.float32).astype(jnp.bfloat16)
    values = values.reshape(key_rows, head_local, -1)
    scores = jnp.einsum("qhd,khd->hqk", query_nope, key_proj, preferred_element_type=jnp.float32)
    scores = scores + jnp.einsum(
        "qhr,kr->hqk", query_rot, pe_block, preferred_element_type=jnp.float32
    )
    return (scores * (NOPE + ROPE) ** (-0.5), values)


def absorb(running, scores, values):
    top_old, sum_old, acc_old = running
    top_new = jnp.maximum(top_old, jnp.max(scores, axis=-1))
    factor = jnp.exp(top_old - top_new)
    exp_terms = jnp.exp(scores - top_new[:, :, None])
    sum_new = sum_old * factor + jnp.sum(exp_terms, axis=-1)
    update = jnp.einsum(
        "hqk,khd->qhd", exp_terms.astype(jnp.bfloat16), values, preferred_element_type=jnp.float32
    )
    return (top_new, sum_new, acc_old * factor.T[:, :, None] + update)


def slot_targets(route_ids, expert_total, capacity):
    pair_ids = route_ids.reshape(route_ids.shape[:-2] + (-1,))
    onehot = (pair_ids[..., None] == jnp.arange(expert_total, dtype=jnp.int32)).astype(jnp.int32)
    earlier = jnp.cumsum(onehot, axis=-2) - onehot
    return pair_ids * capacity + jnp.sum(earlier * onehot, axis=-1)


def dispatch_matrix(targets, tok_rows, top_k, slot_total):
    matches = targets[..., None, :] == jnp.arange(slot_total, dtype=jnp.int32)[:, None]
    matches = matches.reshape(matches.shape[:-1] + (tok_rows, top_k))
    return jnp.any(matches, axis=-1).astype(jnp.bfloat16)


def on_device(
    q_latent,
    kv_latent,
    rope_key,
    gain_query,
    gain_latent,
    w_query,
    w_key,
    w_value,
    w_out,
    tokens_b,
    gain_norm,
    routes,
    route_weights,
    shared_gate,
    shared_up,
    shared_down,
    expert_gate,
    expert_up,
    expert_down,
):
    tok_rows = q_latent.shape[0]
    tp_count = lax.axis_size("tp")
    ep_count = lax.axis_size("ep")
    group_rows = tok_rows * tp_count
    seq_span = ep_count // SEQS
    local_rank = lax.axis_index("ep") % seq_span
    head_local = w_value.shape[1] // VDIM
    q_normed = rms_scale(q_latent, gain_query)
    kv_normed = rms_scale(kv_latent, gain_latent)
    frequency_cos, frequency_sin = rope_angles(
        local_rank * group_rows
        + lax.axis_index("tp") * tok_rows
        + jnp.arange(tok_rows, dtype=jnp.int32),
        ROPE,
    )
    rot_own = rotate_pairs(rope_key.astype(jnp.float32), frequency_cos, frequency_sin)
    latent = jnp.concatenate([kv_normed, rot_own.astype(jnp.bfloat16)], axis=1)

    top_k = routes.shape[1]
    model_width = tokens_b.shape[1]
    exp_dev = expert_gate.shape[0]
    expert_total = exp_dev * ep_count
    capacity = 5 * tok_rows * top_k // (4 * expert_total)
    slot_total = expert_total * capacity
    normed_b = rms_scale(tokens_b, gain_norm)
    own_targets = slot_targets(routes, expert_total, capacity)
    mapping = dispatch_matrix(own_targets, tok_rows, top_k, slot_total)
    outgoing = jnp.dot(mapping, normed_b, preferred_element_type=jnp.float32).astype(jnp.bfloat16)
    outgoing = outgoing.reshape(ep_count, exp_dev * capacity, model_width)
    incoming = exchange(outgoing, "ep", 1)

    shared_rows = lax.all_gather(normed_b, "tp", axis=0, tiled=True)
    group_q = lax.all_gather(q_normed, "tp", axis=0, tiled=True)
    all_latent = lax.all_gather(latent, ("ep", "tp"), axis=0, tiled=True)
    arrived = lax.all_gather(incoming, "tp", axis=0, tiled=True)

    positions = local_rank * group_rows + jnp.arange(group_rows, dtype=jnp.int32)
    cos_tab, sin_tab = rope_angles(positions, ROPE)
    query_full = jnp.dot(group_q, w_query, preferred_element_type=jnp.float32)
    query_full = query_full.reshape(group_rows, head_local, NOPE + ROPE)
    query_rot = rotate_pairs(
        query_full[:, :, NOPE:], cos_tab[:, None, :], sin_tab[:, None, :]
    ).astype(jnp.bfloat16)
    query_nope = query_full[:, :, :NOPE].astype(jnp.bfloat16)

    gate_shared = jnp.dot(shared_rows, shared_gate, preferred_element_type=jnp.float32)
    up_shared = jnp.dot(shared_rows, shared_up, preferred_element_type=jnp.float32)
    shared_hidden = (jax.nn.silu(gate_shared) * up_shared).astype(jnp.bfloat16)
    shared_part = jnp.dot(shared_hidden, shared_down, preferred_element_type=jnp.float32).astype(
        jnp.bfloat16
    )
    shared_parts = exchange(shared_part.reshape(tp_count, tok_rows, model_width), "tp", 3)
    all_latent, shared_parts = lax.optimization_barrier((all_latent, shared_parts))
    shared_result = jnp.sum(shared_parts.astype(jnp.float32), axis=0).astype(jnp.bfloat16)

    first_rank = lax.axis_index("ep") - local_rank
    row_ids = jnp.arange(group_rows, dtype=jnp.int32)

    def attend_block(turn, running):
        block = lax.dynamic_slice_in_dim(
            all_latent, (first_rank + turn) * group_rows, group_rows, axis=0
        )
        scores, values = block_scores(
            query_nope,
            query_rot,
            block[:, : kv_latent.shape[1]],
            block[:, kv_latent.shape[1] :],
            w_key,
            w_value,
            head_local,
        )
        allowed = positions[:, None] >= (turn * group_rows + row_ids)[None, :]
        scores = jnp.where(allowed[None], scores, -jnp.inf)
        return absorb(running, scores, values)

    start_state = (
        jnp.full((head_local, group_rows), -jnp.inf, jnp.float32),
        jnp.zeros((head_local, group_rows), jnp.float32),
        jnp.zeros((group_rows, head_local, VDIM), jnp.float32),
    )
    running = lax.fori_loop(0, local_rank + 1, attend_block, start_state)
    sum_all = running[1]
    acc_all = running[2]
    heads_out = (
        (acc_all / sum_all.T[:, :, None])
        .astype(jnp.bfloat16)
        .reshape(group_rows, head_local * VDIM)
    )
    mixer_part = jnp.dot(heads_out, w_out, preferred_element_type=jnp.float32).astype(
        jnp.bfloat16
    )

    arrived, mixer_part = lax.optimization_barrier((arrived, mixer_part))

    routed = arrived.reshape(tp_count * ep_count, exp_dev, capacity, model_width)
    routed_gate = jnp.einsum(
        "sjcm,jmf->sjcf", routed, expert_gate, preferred_element_type=jnp.float32
    )
    routed_up = jnp.einsum("sjcm,jmf->sjcf", routed, expert_up, preferred_element_type=jnp.float32)
    routed_hidden = (jax.nn.silu(routed_gate) * routed_up).astype(jnp.bfloat16)
    routed_part = jnp.einsum(
        "sjcf,jfm->sjcm", routed_hidden, expert_down, preferred_element_type=jnp.float32
    ).astype(jnp.bfloat16)
    routed_part = routed_part.reshape(tp_count * slot_total, model_width)
    routed_back = lax.psum_scatter(routed_part, "tp", scatter_dimension=0, tiled=True)
    mixer_out = lax.psum_scatter(mixer_part, "tp", scatter_dimension=0, tiled=True)
    returned = exchange(routed_back.reshape(ep_count, exp_dev * capacity, model_width), "ep", 2)
    returned = returned.reshape(slot_total, model_width)
    hits = own_targets.reshape(tok_rows, top_k)[:, :, None] == jnp.arange(
        slot_total, dtype=jnp.int32
    )
    combine = jnp.sum(jnp.where(hits, route_weights[:, :, None], 0.0), axis=1)
    routed_sum = jnp.zeros((tok_rows, model_width), jnp.float32)
    for _ in range(3):
        term = lax.reduce_precision(combine, 8, 7)
        routed_sum = routed_sum + jnp.dot(
            term.astype(jnp.bfloat16), returned, preferred_element_type=jnp.float32
        )
        combine = combine - term
    expert_mix = (shared_result.astype(jnp.float32) + routed_sum).astype(jnp.bfloat16)
    return (mixer_out, expert_mix)


def solution(mesh):
    return jax.shard_map(
        on_device,
        mesh=mesh,
        in_specs=(
            P(("ep", "tp"), None),
            P(("ep", "tp"), None),
            P(("ep", "tp"), None),
            P(),
            P(),
            P(None, "tp"),
            P(None, "tp"),
            P(None, "tp"),
            P("tp", None),
            P(("ep", "tp"), None),
            P(),
            P(("ep", "tp"), None),
            P(("ep", "tp"), None),
            P(None, "tp"),
            P(None, "tp"),
            P("tp", None),
            P("ep", None, "tp"),
            P("ep", None, "tp"),
            P("ep", "tp", None),
        ),
        out_specs=(P(("ep", "tp"), None), P(("ep", "tp"), None)),
        check_vma=False,
    )
```
